512 devices in a mesh: grp: 2 (over y), sp: 16 (over z), tp: 16 (over x, core).
Axes of the slice: x: 8, y: 2, z: 16, core: 2. Of those that a mesh axis runs over, the one named last changes fastest.
The devices are a block of a 8x8x16 slice.
Arguments:
- target: bfloat16 [4096, 2048], P(('grp', 'sp', 'tp')), parts along dimension 0, may hold values from -5 to 5
- source: bfloat16 [32768, 2048], P(('grp', 'sp', 'tp')), parts along dimension 0, may hold values from -5 to 5
- source_gain: float32 [2048], replicated, may hold values from 0.1 to 1.9
- pre_first: float32 [2048], replicated, may hold values from 0.1 to 1.9
- query_first: bfloat16 [2048, 2048], P(None, 'tp')
- keyval_first: bfloat16 [2048, 1024], P(None, 'tp')
- out_first: bfloat16 [2048, 2048], P('tp'), may hold values from -0.125 to 0.125
- post_first: float32 [2048], replicated, may hold values from 0.1 to 1.9
- ffn_pre: float32 [2048], replicated, may hold values from 0.1 to 1.9
- w_gate: bfloat16 [2048, 2816], P(None, 'tp'), may hold values from -0.125 to 0.125
- w_value: bfloat16 [2048, 2816], P(None, 'tp'), may hold values from -0.125 to 0.125
- conv_gate: float32 [3, 2816], P(None, 'tp'), may hold values from -3.5 to 3.5
- conv_value: float32 [3, 2816], P(None, 'tp'), may hold values from -3.5 to 3.5
- w_down: bfloat16 [2816, 2048], P('tp'), may hold values from -0.109375 to 0.109375
- ffn_post: float32 [2048], replicated, may hold values from 0.1 to 1.9
- pre_second: float32 [2048], replicated, may hold values from 0.1 to 1.9
- query_second: bfloat16 [2048, 2048], P(None, 'tp')
- keyval_second: bfloat16 [2048, 1024], P(None, 'tp')
- out_second: bfloat16 [2048, 2048], P('tp'), may hold values from -0.125 to 0.125
- post_second: float32 [2048], replicated, may hold values from 0.1 to 1.9
Outputs:
- decoded: float32 [4096, 2048], P(('grp', 'sp', 'tp')), parts along dimension 0
The draws below stay inside these ranges and needn't reach their ends.
There are 2 independent parts, one for each index of `grp`. The reference program is written for one: setup_inputs(seed, part) draws one part's arguments, and reference() takes and returns one part's arrays. A program takes and returns all parts, laid end to end along the dimension named above; an argument that names none is the same for every part. Nothing has to cross between parts.
All inputs are finite; a program needn't handle non-finite values.
Results may differ from the reference program's by a relative error of at most 0.04.
Values may be sent and summed in bfloat16 or wider, within the bound.
A program may use at most 128 MiB of HBM per device.

```python
import jax
import jax.numpy as jnp
from jax import lax

D = 2048
HEAD = 128
QH = 16
KVH = 4
FF = 2816
TARGET = 2048
SOURCE = 16384
N_TP = 16


def draw_target(key, part):
    rows = jnp.clip(jax.random.normal(jax.random.fold_in(key, 11), (TARGET, D), jnp.float32), -5.0, 5.0)
    return rows.astype(jnp.bfloat16)


def draw_source(key, part):
    rows = jnp.clip(jax.random.normal(jax.random.fold_in(key, 12), (SOURCE, D), jnp.float32), -5.0, 5.0)
    return rows.astype(jnp.bfloat16)


def layer_weights(key, salt):
    drawn_query = jax.random.normal(jax.random.fold_in(key, salt + 1), (D, QH * HEAD), jnp.float32) * D ** (-0.5)
    drawn_keyval = jax.random.normal(jax.random.fold_in(key, salt + 2), (D, KVH, 2, HEAD), jnp.float32) * D ** (-0.5)
    return (drawn_query, drawn_keyval.reshape(D, KVH * 2 * HEAD))


def draw_query_first(key, part):
    return layer_weights(key, 41)[0].astype(jnp.bfloat16)


def draw_keyval_first(key, part):
    return layer_weights(key, 41)[1].astype(jnp.bfloat16)


def draw_query_second(key, part):
    return layer_weights(key, 51)[0].astype(jnp.bfloat16)


def draw_keyval_second(key, part):
    return layer_weights(key, 51)[1].astype(jnp.bfloat16)


def block_levels(stream_key, dims, cuts, smallest, top_value):
    loudness, own = 1.0, jax.random.fold_in(stream_key, 6)
    for dim, shards_of in cuts:
        draws = jnp.exp(jax.random.uniform(jax.random.fold_in(own, dim), (shards_of,), jnp.float32, smallest / len(cuts), top_value / len(cuts)))
        loudness = loudness * jnp.repeat(draws, dims[dim] // shards_of).reshape([-1 if axis == dim else 1 for axis in range(len(dims))])
    return loudness


def bell_draw(own_key, shape, scale, bound, split=(), held_as=jnp.bfloat16):
    result = jax.random.normal(own_key, shape, jnp.float32) * scale
    if len(split) > 0:
        result = block_levels(own_key, shape, split, -0.22, 0.18) * result
    return jnp.clip(result, min=-bound, max=bound).astype(held_as)


def setup_inputs(seed: int = 0, part: int = 0) -> dict:
    key_of = jax.random.split(jax.random.key(seed), 21)
    part_splits = jax.random.split(jax.random.fold_in(key_of[20], part), 21)
    return {
        "target": draw_target(jax.random.fold_in(jax.random.fold_in(key_of[20], part), 71), part),
        "source": draw_source(jax.random.fold_in(jax.random.fold_in(key_of[20], part), 71), part),
        "source_gain": jnp.clip(jax.random.uniform(key_of[2], (D,), jnp.float32, 0.1, 1.9), 0.1, 1.9),
        "pre_first": jnp.clip(jax.random.uniform(key_of[3], (D,), jnp.float32, 0.1, 1.9), 0.1, 1.9),
        "query_first": draw_query_first(jax.random.fold_in(key_of[20], 71), part),
        "keyval_first": draw_keyval_first(jax.random.fold_in(key_of[20], 71), part),
        "out_first": bell_draw(key_of[6], (QH * HEAD, D), (QH * HEAD) ** -0.5, 0.125, ((0, 16),)),
        "post_first": jnp.clip(jax.random.uniform(key_of[7], (D,), jnp.float32, 0.1, 1.9), 0.1, 1.9),
        "ffn_pre": jnp.clip(jax.random.uniform(key_of[8], (D,), jnp.float32, 0.1, 1.9), 0.1, 1.9),
        "w_gate": bell_draw(key_of[9], (D, FF), D ** -0.5, 0.125, ((1, 16),)),
        "w_value": bell_draw(key_of[10], (D, FF), D ** -0.5, 0.125, ((1, 16),)),
        "conv_gate": bell_draw(key_of[11], (3, FF), 3 ** -0.5, 3.5, ((1, 16),), jnp.float32),
        "conv_value": bell_draw(key_of[12], (3, FF), 3 ** -0.5, 3.5, ((1, 16),), jnp.float32),
        "w_down": bell_draw(key_of[13], (FF, D), FF ** -0.5, 0.109375, ((0, 16),)),
        "ffn_post": jnp.clip(jax.random.uniform(key_of[14], (D,), jnp.float32, 0.1, 1.9), 0.1, 1.9),
        "pre_second": jnp.clip(jax.random.uniform(key_of[15], (D,), jnp.float32, 0.1, 1.9), 0.1, 1.9),
        "query_second": draw_query_second(jax.random.fold_in(key_of[20], 71), part),
        "keyval_second": draw_keyval_second(jax.random.fold_in(key_of[20], 71), part),
        "out_second": bell_draw(key_of[18], (QH * HEAD, D), (QH * HEAD) ** -0.5, 0.125, ((0, 16),)),
        "post_second": jnp.clip(jax.random.uniform(key_of[19], (D,), jnp.float32, 0.1, 1.9), 0.1, 1.9),
    }


def normed(values, gain):
    widened = values.astype(jnp.float32)
    return widened * lax.rsqrt(lax.optimization_barrier(jnp.mean(widened * widened, axis=-1, keepdims=True)) + 1e-06) * gain

def sharded_product(left_side, right_side, shards):
    column_span = left_side.shape[1] // shards

    def accumulate(running, shard_index):
        left_part = lax.dynamic_slice_in_dim(left_side, shard_index * column_span, column_span, 1)
        right_part = lax.dynamic_slice_in_dim(right_side, shard_index * column_span, column_span, 0)
        rounded = jnp.dot(left_part, right_part, preferred_element_type=jnp.float32).astype(jnp.bfloat16)
        rounded = lax.optimization_barrier(rounded)
        return (running + rounded.astype(jnp.float32), None)
    initial = jnp.zeros((left_side.shape[0], right_side.shape[1]), jnp.float32)
    summed, unused = lax.scan(accumulate, initial, jnp.arange(shards, dtype=jnp.int32))
    return summed

def attend(queries, keyvals):
    group_size = QH // KVH
    scale_factor = HEAD ** (-0.5)
    query_heads = jnp.moveaxis(queries.reshape(TARGET, QH, HEAD), 1, 0)

    def one_head(inputs):
        head_queries, head_index = inputs
        columns = lax.dynamic_slice_in_dim(keyvals, head_index // group_size * (2 * HEAD), 2 * HEAD, 1)
        head_keys = columns[:, :HEAD]
        head_values = columns[:, HEAD:]
        scores = lax.dot_general(head_queries, head_keys, (((1,), (1,)), ((), ())), preferred_element_type=jnp.float32) * scale_factor
        row_max = lax.optimization_barrier(jnp.max(scores, axis=1, keepdims=True))
        weights = jnp.exp(scores - row_max)
        weight_sum = lax.optimization_barrier(jnp.sum(weights, axis=1, keepdims=True))
        gathered = jnp.dot(weights.astype(jnp.bfloat16), head_values, preferred_element_type=jnp.float32)
        return (gathered / weight_sum).astype(jnp.bfloat16)
    outputs = lax.map(one_head, (query_heads, jnp.arange(QH, dtype=jnp.int32)))
    return jnp.moveaxis(outputs, 0, 1).reshape(TARGET, QH * HEAD)

def attention_layer(stream, pre_gain, w_query, keyvals, w_out, post_gain):
    hidden = normed(stream, pre_gain).astype(jnp.bfloat16)
    queries = jnp.dot(hidden, w_query, preferred_element_type=jnp.float32).astype(jnp.bfloat16)
    heads = attend(queries, keyvals)
    mixed = sharded_product(heads, w_out, N_TP)
    return stream.astype(jnp.float32) + normed(mixed, post_gain)

def causal_mix(up_rows, conv_taps):
    padded = jnp.pad(up_rows.astype(jnp.float32), ((2, 0), (0, 0)))
    length = up_rows.shape[0]
    return conv_taps[0] * padded[:length] + conv_taps[1] * padded[1:length + 1] + conv_taps[2] * padded[2:]

def reference(target, source, source_gain, pre_first, query_first, keyval_first, out_first, post_first, ffn_pre, w_gate, w_value, conv_gate, conv_value, w_down, ffn_post, pre_second, query_second, keyval_second, out_second, post_second):
    source_normed = normed(source, source_gain).astype(jnp.bfloat16)
    kv_first = jnp.dot(source_normed, keyval_first, preferred_element_type=jnp.float32).astype(jnp.bfloat16)
    kv_second = jnp.dot(source_normed, keyval_second, preferred_element_type=jnp.float32).astype(jnp.bfloat16)
    after_first = attention_layer(target, pre_first, query_first, kv_first, out_first, post_first)
    ffn_input = normed(after_first, ffn_pre).astype(jnp.bfloat16)
    up_gate = jnp.dot(ffn_input, w_gate, preferred_element_type=jnp.float32).astype(jnp.bfloat16)
    up_value = jnp.dot(ffn_input, w_value, preferred_element_type=jnp.float32).astype(jnp.bfloat16)
    gated = (jax.nn.gelu(causal_mix(up_gate, conv_gate), approximate=True) * causal_mix(up_value, conv_value)).astype(jnp.bfloat16)
    ffn_sum = sharded_product(gated, w_down, N_TP)
    after_ffn = after_first + normed(ffn_sum, ffn_post)
    return attention_layer(after_ffn, pre_second, query_second, kv_second, out_second, post_second)
```

```python
import functools
import math

import jax
import jax.numpy as jnp
from jax import lax
from jax.experimental import pallas as pl
from jax.experimental.pallas import tpu as pltpu
from jax.sharding import PartitionSpec as P

HEAD = 128
KVH = 4
CORES = 2
SUBS = 4
MESH = pl.DeviceIdType.MESH
F32 = jnp.float32
BF16 = jnp.bfloat16


def normed(v, gain):
    return v * lax.rsqrt(jnp.mean(v * v, axis=-1, keepdims=True) + 1e-6) * gain


def dot(a, b, contract=((1,), (0,))):
    return lax.dot_general(a, b, (contract, ((), ())), preferred_element_type=F32)


def kernel(
    nx, nz,
    tgt_hbm, src_hbm, taps_hbm, sgain, pre1, post1, fpre, fpost, pre2, post2,
    q1_hbm, q2_hbm, kv1_hbm, kv2_hbm, o1_hbm, o2_hbm, wg_hbm, wv_hbm, wd_hbm,
    out_ref,
    src_v, tgt_v, kvin, w2, wq, wo, wgv, wdn, taps,
    rows_x, kv_st, kvb, hb, sb, rb, qb, o_st, ob, s_st, st, acc, m_run, l_run, up, rim, resid,
    loc_sem, w_send, w_recv, x_send, x_recv, e_send, e_recv, z_send, z_recv,
    ag_send, ag_recv, rs_send, rs_recv, q_send, q_recv, o_send, o_recv, s_send, s_recv, r_send, r_recv,
):
    z = lax.axis_index("sp")
    tp = lax.axis_index("tp")
    x, c = tp // CORES, tp % CORES
    half = x % 2
    idx = half * CORES + c
    group = tp - idx
    gsize = nx * CORES // KVH
    src_rows = src_v.shape[0]
    tgt_rows = tgt_v.shape[0]
    sub_rows = src_rows // 2
    block = kvb.shape[3]
    hops = nz // 2
    width = nx * tgt_rows
    scale2 = HEAD ** -0.5 * math.log2(math.e)

    def chip(k):
        return lax.rem(x + k + nx, nx)

    def same_core(k):
        return {"tp": chip(k) * CORES + c}

    partner = {"tp": tp + 1 - 2 * c}
    across = {"tp": (x + 1 - 2 * half) * CORES + c}

    def zpos(k):
        return lax.rem(z + k + nz, nz)

    def remote(src, dst, ss, rs, dev):
        return pltpu.make_async_remote_copy(
            src_ref=src, dst_ref=dst, send_sem=ss, recv_sem=rs, device_id=dev, device_id_type=MESH
        )

    loads = [
        (src_hbm, src_v), (kv1_hbm, kvin.at[0]), (kv2_hbm, kvin.at[1]), (tgt_hbm, tgt_v),
        (q1_hbm, wq.at[0, c]), (o1_hbm, wo.at[0, c]), (wg_hbm, wgv.at[0, c]), (wv_hbm, wgv.at[1, c]),
        (wd_hbm, wdn.at[c]), (taps_hbm, taps.at[c]), (q2_hbm, wq.at[1, c]), (o2_hbm, wo.at[1, c]),
    ]
    local = [pltpu.make_async_copy(a, b, loc_sem.at[i]) for i, (a, b) in enumerate(loads)]
    for cp in local:
        cp.start()

    barrier = pltpu.get_barrier_semaphore()
    peers = [same_core(k) for k in range(1, nx)]
    peers += [{"tp": group + lax.rem(idx + r, gsize)} for r in range(1, gsize)]
    peers += [{"sp": zpos(1)}, {"sp": zpos(-1)}, {"sp": zpos(2 * c - 1), "tp": tp + 1 - 2 * c}]
    for dev in peers:
        pl.semaphore_signal(barrier, inc=1, device_id=dev, device_id_type=MESH)

    local[0].wait()
    rows = normed(src_v[...].astype(F32), sgain[...]).astype(BF16)
    rows_x[x, 0] = rows[:sub_rows]
    rows_x[x, 1] = rows[sub_rows:]
    local[1].wait()
    local[2].wait()
    w2[c] = jnp.concatenate([kvin[0], kvin[1]], axis=1)
    local[3].wait()
    hb[0, x] = normed(tgt_v[...].astype(F32), pre1[...]).astype(BF16)
    pl.semaphore_wait(barrier, len(peers))

    def x_copy(d, h, s, origin):
        ref = rows_x.at[origin, s]
        return remote(ref, ref, x_send.at[d, h, s], x_recv.at[d, h, s], same_core(1 - 2 * d))

    for s in range(2):
        for d in range(2):
            x_copy(d, 0, s, x).start()

    weights = [
        (w2.at[c], w2.at[c]), (q1_hbm, wq.at[0, c]), (o1_hbm, wo.at[0, c]), (wg_hbm, wgv.at[0, c]),
        (wv_hbm, wgv.at[1, c]), (wd_hbm, wdn.at[c]), (taps_hbm, taps.at[c]), (q2_hbm, wq.at[1, c]),
        (o2_hbm, wo.at[1, c]),
    ]
    w_copies = [remote(a, b, w_send.at[i], w_recv.at[i], partner) for i, (a, b) in enumerate(weights)]
    w_copies[0].start()

    def project(chunk):
        left = dot(chunk, w2[0])
        right = dot(chunk, w2[1])
        w = HEAD // 2
        return [
            jnp.concatenate([left[:, l * w : (l + 1) * w], right[:, l * w : (l + 1) * w]], axis=1).astype(BF16)
            for l in range(2)
        ]

    def place(outs, origin, at):
        per = nx // 2
        for l in range(2):
            kv_st[origin // per, l, pl.ds(pl.multiple_of(lax.rem(origin, per) * src_rows, src_rows), src_rows), :] = (
                outs[l][at : at + src_rows]
            )

    def two_subs(origin):
        return [rows_x[origin, 0], rows_x[origin, 1]]

    w_copies[0].wait_recv()
    place(project(jnp.concatenate(two_subs(x), axis=0)), x, 0)

    far = nx // 2

    def x_hop(h, last):
        right_o, left_o = chip(-h), chip(h)
        for s in range(2):
            x_copy(0, h - 1, s, right_o).wait_recv()
            if not last or s == 0:
                x_copy(0, h, s, right_o).start()
            x_copy(1, h - 1, s, left_o).wait_recv()
            if not last or s == 1:
                x_copy(1, h, s, left_o).start()
        outs = project(jnp.concatenate(two_subs(right_o) + two_subs(left_o), axis=0))
        place(outs, right_o, 0)
        place(outs, left_o, src_rows)

    for h in range(1, far):
        x_hop(h, h == far - 1)
        for cp in w_copies[3 * h - 2 : 3 * h + 1]:
            cp.start()
    for cp in w_copies[3 * far - 2 :]:
        cp.start()
    x_copy(0, far - 1, 0, chip(far)).wait_recv()
    x_copy(1, far - 1, 1, chip(far)).wait_recv()
    place(project(jnp.concatenate(two_subs(chip(far)), axis=0)), chip(far), 0)

    e_copies = [
        remote(kv_st.at[1 - half, l], kvb.at[l, z, half], e_send.at[l], e_recv.at[l], across) for l in range(2)
    ]
    for cp in e_copies:
        cp.start()
    for l in range(2):
        kvb[l, z, half] = kv_st[half, l]

    order = sorted(range(1, nx), key=lambda k: -min(k, nx - k))

    def ag_copy(ph, k):
        return remote(hb.at[ph, x], hb.at[ph, x], ag_send.at[ph, k], ag_recv.at[ph, k], same_core(k))

    def ag_start(ph):
        for k in order:
            ag_copy(ph, k).start()

    def ag_wait(ph):
        for k in order:
            ref = hb.at[ph, chip(-k)]
            remote(ref, ref, ag_send.at[ph, k], ag_recv.at[ph, k], same_core(k)).wait_recv()
        return hb[ph].astype(F32).reshape(width, -1).astype(BF16)

    def rs_copy(ph, k):
        return remote(sb.at[ph, chip(k)], rb.at[ph, x], rs_send.at[ph, k], rs_recv.at[ph, k], same_core(k))

    def rs_start(ph, total):
        sb[ph] = total.reshape(nx, tgt_rows, -1).astype(BF16)
        for k in order:
            rs_copy(ph, k).start()
        rb[ph, x] = sb[ph, x]

    def rs_wait(ph):
        for k in order:
            remote(sb.at[ph, chip(k)], rb.at[ph, chip(-k)], rs_send.at[ph, k], rs_recv.at[ph, k], same_core(k)).wait_recv()
        return jnp.sum(rb[ph].astype(F32), axis=0)

    piece = block // 2

    def z_copy(l, d, h, s, origin):
        kind = lax.rem(half + s // 2, 2)
        ref = kvb.at[l, origin, kind, pl.ds((s % 2) * piece, piece)]
        return remote(ref, ref, z_send.at[l, d, h, s], z_recv.at[l, d, h, s], {"sp": zpos(1 - 2 * d)})

    def z_start(l, s):
        for d in range(2):
            z_copy(l, d, 0, s, z).start()

    def z_hop(l, h, last):
        right_o, left_o = zpos(-h), zpos(h)
        for s in range(SUBS):
            for d, origin in ((0, right_o), (1, left_o)):
                z_copy(l, d, h - 1, s, origin).wait_recv()
                if not last or s // 2 == d:
                    z_copy(l, d, h, s, origin).start()

    def z_last(l):
        for s in range(SUBS):
            z_copy(l, s // 2, hops - 1, s, zpos(hops)).wait_recv()

    z_start(0, 0)
    z_start(0, 1)
    ag_start(0)
    e_copies[0].wait_recv()
    z_start(0, 2)
    z_start(0, 3)
    e_copies[1].wait_recv()

    def q_slot(l, i):
        return qb.at[l, i]

    def q_copy(l, r):
        return remote(
            qb.at[l, idx], qb.at[l, idx], q_send.at[l, r], q_recv.at[l, r], {"tp": group + lax.rem(idx + r, gsize)}
        )

    def q_project(l, hidden):
        for hh in range(CORES):
            qb[l, idx, hh * width : (hh + 1) * width, :] = dot(hidden, wq[l, hh]).astype(BF16)
        for r in range(1, gsize):
            q_copy(l, r).start()

    def q_wait(l):
        for r in range(1, gsize):
            ref = qb.at[l, lax.rem(idx + gsize - r, gsize)]
            remote(ref, ref, q_send.at[l, r], q_recv.at[l, r], {"tp": group}).wait_recv()
        m_run[...] = jnp.full_like(m_run, -jnp.inf)
        l_run[...] = jnp.zeros_like(l_run)
        acc[...] = jnp.zeros_like(acc)

    def absorb(l, keys, values):
        queries = qb[l].reshape(gsize * CORES * width, HEAD)
        scores = dot(keys, queries, ((1,), (1,)))
        m_old = m_run[...]
        m_new = jnp.maximum(m_old, jnp.max(scores, axis=0, keepdims=True))
        rescale = jnp.exp2((m_old - m_new) * scale2)
        weights = jnp.exp2((scores - m_new) * scale2)
        l_run[...] = l_run[...] * rescale + jnp.sum(weights, axis=0, keepdims=True)
        acc[...] = acc[...] * rescale + dot(values, weights.astype(BF16), ((0,), (0,)))
        m_run[...] = m_new

    def absorb_pair(l, a, b):
        absorb(
            l,
            jnp.concatenate([kvb[l, a, 0], kvb[l, b, 0]], axis=0),
            jnp.concatenate([kvb[l, a, 1], kvb[l, b, 1]], axis=0),
        )

    def o_copies(l, r):
        to = lax.rem(idx + r, gsize)
        dev = {"tp": group + to}
        return [
            remote(o_st.at[l, to], ob.at[l, idx], o_send.at[l, r], o_recv.at[l, r], dev),
            remote(s_st.at[l, to], st.at[l, idx], s_send.at[l, r], s_recv.at[l, r], dev),
        ]

    def o_start(l):
        total = l_run[...]
        share = (acc[...] / total).astype(BF16)
        cols = CORES * width
        for i in range(gsize):
            at = slice(i * cols, (i + 1) * cols)
            o_st[l, i] = share[:, at]
            s_st[l, i] = jnp.concatenate(
                [m_run[:, at], total[:, at], jnp.zeros((6, cols), F32)], axis=0
            )
        for r in range(1, gsize):
            for cp in o_copies(l, r):
                cp.start()
        ob[l, idx] = o_st[l, idx]
        st[l, idx] = s_st[l, idx]

    def o_wait(l):
        for r in range(1, gsize):
            at = lax.rem(idx + gsize - r, gsize)
            remote(o_st.at[l, at], ob.at[l, at], o_send.at[l, r], o_recv.at[l, r], {"tp": group}).wait_recv()
            remote(s_st.at[l, at], st.at[l, at], s_send.at[l, r], s_recv.at[l, r], {"tp": group}).wait_recv()
        maxima = [st[l, i, 0:1, :] for i in range(gsize)]
        top = functools.reduce(jnp.maximum, maxima)
        shares = [st[l, i, 1:2, :] * jnp.exp2((maxima[i] - top) * scale2) for i in range(gsize)]
        whole = functools.reduce(jnp.add, shares)
        mixed = functools.reduce(jnp.add, [ob[l, i].astype(F32) * shares[i] for i in range(gsize)])
        heads = (mixed / whole).T.astype(BF16)
        return sum(dot(heads[hh * width : (hh + 1) * width], wo[l, hh]) for hh in range(CORES))

    for h in range(1, 3):
        z_hop(0, h, False)
    hidden = ag_wait(0)
    local[4].wait()
    w_copies[1].wait_recv()
    q_project(0, hidden)
    z_hop(0, 3, False)
    q_wait(0)
    absorb(0, kvb[0, z, 0], kvb[0, z, 1])

    def early(h, carry):
        absorb_pair(0, zpos(-h), zpos(h))
        return carry

    lax.fori_loop(1, 3, early, 0)

    def body(h, carry):
        z_hop(0, h, False)
        absorb_pair(0, zpos(1 - h), zpos(h - 1))
        return carry

    lax.fori_loop(4, hops - 1, body, 0)
    z_hop(0, hops - 1, True)
    for s in range(SUBS):
        z_start(1, s)
    absorb_pair(0, zpos(2 - hops), zpos(hops - 2))
    absorb_pair(0, zpos(1 - hops), zpos(hops - 1))
    z_last(0)
    absorb(0, kvb[0, zpos(hops), 0], kvb[0, zpos(hops), 1])

    o_start(0)
    z_hop(1, 1, False)
    local[5].wait()
    w_copies[2].wait_recv()
    rs_start(0, o_wait(0))
    z_hop(1, 2, False)
    after_first = tgt_v[...].astype(F32) + normed(rs_wait(0), post1[...])
    hb[1, x] = normed(after_first, fpre[...]).astype(BF16)
    ag_start(1)
    resid[...] = after_first
    z_hop(1, 3, False)
    for i in (6, 7, 8, 9):
        local[i].wait()
    for i in (3, 4, 5, 6):
        w_copies[i].wait_recv()
    hidden = ag_wait(1)
    units = wdn.shape[1]
    span = up.shape[2] // 4
    for kind in range(2):
        for core in range(CORES):
            at = (kind * CORES + core) * span
            up[:, :, at : at + units] = dot(hidden, wgv[kind, core]).reshape(nx, tgt_rows, units).astype(BF16)
    rim_a = remote(up.at[pl.ds(0, nx - 1)], rim.at[pl.ds(c, nx - 1)], r_send.at[0], r_recv.at[0], partner)
    rim_a.start()
    last_slot = (nx - 1) * (1 - c)
    rim_b = remote(
        up.at[nx - 1], rim.at[last_slot], r_send.at[1], r_recv.at[1], {"sp": zpos(c), "tp": tp + 1 - 2 * c}
    )
    sends_b = jnp.logical_or(c == 0, z < nz - 1)
    gets_b = jnp.logical_or(c == 1, z > 0)

    @pl.when(sends_b)
    def _():
        rim_b.start()

    @pl.when(jnp.logical_not(gets_b))
    def _():
        rim[0] = jnp.zeros(rim.shape[1:], rim.dtype)

    z_hop(1, 4, False)
    rim_a.wait_recv()

    @pl.when(gets_b)
    def _():
        rim_b.wait_recv()

    def conv(kind, core):
        at = (kind * CORES + core) * span
        here = up[:, :, at : at + units].astype(F32)
        before = rim[:, :, at : at + units].astype(F32)
        t = taps[core][3 * kind : 3 * kind + 3, :units]
        one = jnp.concatenate([before[:, -1:], here[:, :-1]], axis=1)
        two = jnp.concatenate([before[:, -2:], here[:, :-2]], axis=1)
        return t[0:1] * two + t[1:2] * one + t[2:3] * here

    total = 0.0
    for core in range(CORES):
        gated = jax.nn.gelu(conv(0, core), approximate=True) * conv(1, core)
        total += dot(gated.reshape(width, units).astype(BF16), wdn[core])
    rs_start(1, total)
    z_hop(1, 5, False)
    after_ffn = resid[...] + normed(rs_wait(1), fpost[...])
    hb[2, x] = normed(after_ffn, pre2[...]).astype(BF16)
    ag_start(2)
    resid[...] = after_ffn
    z_hop(1, 6, False)
    hidden = ag_wait(2)
    local[10].wait()
    w_copies[7].wait_recv()
    q_project(1, hidden)
    z_hop(1, 7, True)
    z_last(1)
    q_wait(1)
    together = 4

    def chunk(i, carry):
        part = kvb[1, pl.ds(i * together, together)]
        absorb(1, part[:, 0].reshape(together * block, HEAD), part[:, 1].reshape(together * block, HEAD))
        return carry

    lax.fori_loop(0, nz // together, chunk, 0)
    o_start(1)
    local[11].wait()
    w_copies[8].wait_recv()
    rs_start(2, o_wait(1))
    out_ref[...] = resid[...] + normed(rs_wait(2), post2[...])

    for h in range(far):
        for s in range(2):
            for d in range(2):
                if h < far - 1 or s == d:
                    x_copy(d, h, s, x).wait_send()
    for cp in w_copies + e_copies:
        cp.wait_send()
    for l in range(2):

        def drained(h, carry):
            for s in range(SUBS):
                for d in range(2):
                    z_copy(l, d, h, s, z).wait_send()
            return carry

        lax.fori_loop(0, hops - 1, drained, 0)
        for s in range(SUBS):
            z_copy(l, s // 2, hops - 1, s, z).wait_send()
        for r in range(1, gsize):
            q_copy(l, r).wait_send()
            for cp in o_copies(l, r):
                cp.wait_send()
    for ph in range(3):
        for k in order:
            ag_copy(ph, k).wait_send()
            rs_copy(ph, k).wait_send()
    rim_a.wait_send()

    @pl.when(sends_b)
    def _():
        rim_b.wait_send()


def solution(mesh):
    nx, nz = mesh.shape["tp"] // CORES, mesh.shape["sp"]
    gsize = nx * CORES // KVH

    def per_device(
        target, source, source_gain, pre_first, query_first, keyval_first, out_first, post_first, ffn_pre,
        w_gate, w_value, conv_gate, conv_value, w_down, ffn_post, pre_second, query_second, keyval_second,
        out_second, post_second,
    ):
        depth = target.shape[1]
        tgt_rows, src_rows = target.shape[0], source.shape[0]
        units = w_gate.shape[1]
        kvw = keyval_first.shape[1]
        width = nx * tgt_rows
        block = nx // 2 * src_rows
        hops = nz // 2
        lanes = -(-units // HEAD) * HEAD
        taps = jnp.pad(jnp.concatenate([conv_gate, conv_value], axis=0), ((0, 2), (0, lanes - units)))
        vmem = pl.BlockSpec(memory_space=pltpu.VMEM)
        anyw = pl.BlockSpec(memory_space=pl.ANY)
        dma = pltpu.SemaphoreType.DMA
        cols = CORES * width
        gains = [g.reshape(1, depth) for g in (source_gain, pre_first, post_first, ffn_pre, ffn_post, pre_second, post_second)]
        return pl.pallas_call(
            functools.partial(kernel, nx, nz),
            out_shape=jax.ShapeDtypeStruct((tgt_rows, depth), F32),
            in_specs=[anyw] * 3 + [vmem] * 7 + [anyw] * 9,
            out_specs=vmem,
            scratch_shapes=[
                pltpu.VMEM((src_rows, depth), BF16),
                pltpu.VMEM((tgt_rows, depth), BF16),
                pltpu.VMEM((2, depth, kvw), BF16),
                pltpu.VMEM((CORES, depth, 2 * kvw), BF16),
                pltpu.VMEM((2, CORES, depth, HEAD), BF16),
                pltpu.VMEM((2, CORES, HEAD, depth), BF16),
                pltpu.VMEM((2, CORES, depth, units), BF16),
                pltpu.VMEM((CORES, units, depth), BF16),
                pltpu.VMEM((CORES, 8, lanes), F32),
                pltpu.VMEM((nx, 2, src_rows // 2, depth), BF16),
                pltpu.VMEM((2, 2, block, HEAD), BF16),
                pltpu.VMEM((2, nz, 2, block, HEAD), BF16),
                pltpu.VMEM((3, nx, tgt_rows, depth), BF16),
                pltpu.VMEM((3, nx, tgt_rows, depth), BF16),
                pltpu.VMEM((3, nx, tgt_rows, depth), BF16),
                pltpu.VMEM((2, gsize, cols, HEAD), BF16),
                pltpu.VMEM((2, gsize, HEAD, cols), BF16),
                pltpu.VMEM((2, gsize, HEAD, cols), BF16),
                pltpu.VMEM((2, gsize, 8, cols), F32),
                pltpu.VMEM((2, gsize, 8, cols), F32),
                pltpu.VMEM((HEAD, gsize * cols), F32),
                pltpu.VMEM((1, gsize * cols), F32),
                pltpu.VMEM((1, gsize * cols), F32),
                pltpu.VMEM((nx, tgt_rows, 4 * lanes), BF16),
                pltpu.VMEM((nx, tgt_rows, 4 * lanes), BF16),
                pltpu.VMEM((tgt_rows, depth), F32),
                dma((12,)),
                dma((9,)), dma((9,)),
                dma((2, nx // 2, 2)), dma((2, nx // 2, 2)),
                dma((2,)), dma((2,)),
                dma((2, 2, hops, SUBS)), dma((2, 2, hops, SUBS)),
                dma((3, nx)), dma((3, nx)),
                dma((3, nx)), dma((3, nx)),
                dma((2, gsize)), dma((2, gsize)),
                dma((2, gsize)), dma((2, gsize)),
                dma((2, gsize)), dma((2, gsize)),
                dma((2,)), dma((2,)),
            ],
            compiler_params=pltpu.CompilerParams(
                collective_id=0, has_side_effects=True, vmem_limit_bytes=56 * 1024 * 1024
            ),
        )(
            target, source, taps, *gains, query_first, query_second, keyval_first, keyval_second,
            out_first, out_second, w_gate, w_value, w_down,
        )

    placed = (
        P(("grp", "sp", "tp"), None), P(("grp", "sp", "tp"), None), P(), P(), P(None, "tp"), P(None, "tp"),
        P("tp", None), P(), P(), P(None, "tp"), P(None, "tp"), P(None, "tp"), P(None, "tp"), P("tp", None),
        P(), P(), P(None, "tp"), P(None, "tp"), P("tp", None), P(),
    )
    return jax.shard_map(
        per_device, mesh=mesh, in_specs=placed, out_specs=P(("grp", "sp", "tp"), None), check_vma=False
    )
```
